32 devices in a mesh: fs: 8 (over z, y), tp: 4 (over x, core).
Axes of the slice: x: 2, y: 2, z: 4, core: 2. Of those that a mesh axis runs over, the one named last changes fastest.
Arguments:
- tokens: bfloat16 [8192, 2048], P('fs', 'tp'), may hold values from -6 to 6
- norm_gain: float32 [2048], P('fs'), may hold values from 0.1 to 1.9
- up_master: float32 [2048, 4096], P('fs', 'tp'), may hold values from -0.125 to 0.125
- down_master: float32 [4096, 2048], P('fs', 'tp'), may hold values from -0.09375 to 0.09375
Outputs:
- mixed: bfloat16 [8192, 2048], P('fs', 'tp')
- up_ready: bfloat16 [2048, 4096], P(None, 'tp')
- down_ready: bfloat16 [4096, 2048], P('tp')
The draws below stay inside these ranges and needn't reach their ends.
All inputs are finite; a program needn't handle non-finite values.
Results may differ from the reference program's by a relative error of at most 0.0095.
Values may be sent and summed in bfloat16 or wider, within the bound.
No kernel may reach another device: no remote copies, remote signals or barrier semaphores. Data moves between devices by JAX's collectives and lax.ppermute only.
A program may use at most 128 MiB of HBM per device.

```python
import jax
import jax.numpy as jnp
from jax import lax

D = 2048
FF = 4096
TOKENS = 8192
N_TP = 4


def steps_of(key, shape, shards, least, high):
    factor_of, own = 1.0, jax.random.fold_in(key, 6)
    for axis_at, blocks in shards:
        steps = jnp.exp(jax.random.uniform(jax.random.fold_in(own, axis_at), (blocks,), jnp.float32, least / len(shards), high / len(shards)))
        factor_of = factor_of * jnp.repeat(steps, shape[axis_at] // blocks).reshape([-1 if axis == axis_at else 1 for axis in range(len(shape))])
    return factor_of


def gaussian(rng, dims, spread, bound, pieces=(), held_as=jnp.bfloat16):
    loudness = steps_of(rng, dims, pieces, -0.22, 0.18) if pieces else 1.0
    array = jax.random.normal(rng, dims, jnp.float32) * spread * loudness
    return jnp.minimum(jnp.maximum(array, -bound), bound).astype(held_as)


def setup_inputs(seed: int = 0) -> dict:
    arg_keys = jax.random.split(jax.random.key(seed), 5)
    tokens = gaussian(arg_keys[0], (TOKENS, D), 1.0, 6.0, ((0, 8), (1, 4)))
    norm_gain = jnp.clip(1.0 + 0.18 * jax.random.normal(arg_keys[1], (D,), jnp.float32), 0.1, 1.9)
    up_master = gaussian(arg_keys[2], (D, FF), D ** -0.5, 0.125, ((0, 8), (1, 4)), jnp.float32)
    down_master = gaussian(arg_keys[3], (FF, D), FF ** -0.5, 0.09375, ((0, 8), (1, 4)), jnp.float32)
    return {"tokens": tokens, "norm_gain": norm_gain, "up_master": up_master, "down_master": down_master}


def reference(tokens, norm_gain, up_master, down_master):
    up_ready = (norm_gain[:, None] * up_master).astype(jnp.bfloat16)
    down_ready = down_master.astype(jnp.bfloat16)
    values = tokens.astype(jnp.float32)
    mean_square = lax.optimization_barrier(jnp.mean(values * values, axis=-1, keepdims=True))
    normed = (values * lax.rsqrt(mean_square + 1e-06)).astype(jnp.bfloat16)
    before = jnp.dot(normed, up_ready, preferred_element_type=jnp.float32)
    hidden = jnp.square(jax.nn.relu(before)).astype(jnp.bfloat16)
    block_size = FF // N_TP
    total = jnp.zeros((tokens.shape[0], D), jnp.float32)
    for block_id in range(N_TP):
        first = block_id * block_size
        partial_value = jnp.dot(hidden[:, first:first + block_size], down_ready[first:first + block_size], preferred_element_type=jnp.float32).astype(jnp.bfloat16)
        partial_value = lax.optimization_barrier(partial_value)
        total = total + partial_value.astype(jnp.float32)
    return (total.astype(jnp.bfloat16), up_ready, down_ready)
```

```python
import jax
import jax.numpy as jnp
from jax import lax
from jax.sharding import PartitionSpec as P


AXES = ("fs", "tp")
BF16, F32 = jnp.bfloat16, jnp.float32


def plain(tokens, norm_gain, up_master, down_master):
    up_local = (norm_gain[:, None] * up_master).astype(BF16)
    up_ready = lax.all_gather(up_local, "fs", axis=0, tiled=True)
    gathered = lax.all_gather(down_master.astype(BF16), "fs", axis=0, tiled=True)
    down_ready = lax.all_to_all(gathered, "tp", split_axis=0, concat_axis=1, tiled=True)
    normed = normalize(lax.all_gather(tokens, "tp", axis=1, tiled=True))
    before = jnp.dot(normed, up_ready, preferred_element_type=F32)
    hidden = jnp.square(jax.nn.relu(before)).astype(BF16)
    part = jnp.dot(hidden, down_ready, preferred_element_type=F32).astype(BF16)
    mixed = lax.psum_scatter(part, "tp", scatter_dimension=1, tiled=True)
    return mixed, up_ready, down_ready


def normalize(features):
    values = features.astype(F32)
    mean_square = jnp.mean(values * values, axis=-1, keepdims=True)
    return (values * lax.rsqrt(mean_square + 1e-06)).astype(BF16)


def routed(n_fs, n_tp):
    n_z = n_fs // 2

    def pairs(move):
        out = []
        for s in range(n_fs * n_tp):
            f, t = divmod(s, n_tp)
            to = move(f // 2, f % 2, t // 2, t % 2)
            if to is not None:
                z, y, x, c = to
                out.append((s, (z * 2 + y) * n_tp + x * 2 + c))
        return out

    over_x = pairs(lambda z, y, x, c: (z, y, 1 - x, c))
    over_y = pairs(lambda z, y, x, c: (z, 1 - y, x, c))
    over_c = pairs(lambda z, y, x, c: (z, y, x, 1 - c))

    def send(value, route):
        return lax.ppermute(value, AXES, route)

    def y_where(keep):
        return pairs(lambda z, y, x, c: (z, 1 - y, x, c) if keep(z) else None)

    def rising(step):
        return pairs(lambda z, y, x, c: (z + 1, y, x, c) if step - 1 <= z < n_z - 1 else None)

    def falling(step):
        return pairs(lambda z, y, x, c: (z - 1, y, x, c) if 1 <= z <= n_z - step else None)

    def shards(tokens, norm_gain, up_master, down_master):
        f, t = lax.axis_index("fs"), lax.axis_index("tp")
        z, y, x, c = f // 2, f % 2, t // 2, t % 2

        up_own = (norm_gain[:, None] * up_master).astype(BF16)
        down_own = down_master.astype(BF16)

        def after(value, *others):
            return lax.optimization_barrier((value,) + others)[0]

        def line(own):
            below, above = [own], [own]
            for step in range(1, n_z):
                below.append(send(below[-1], rising(step)))
                above.append(send(above[-1], falling(step)))
            return below, above

        def put(buf, value, at):
            return lax.dynamic_update_slice(buf, value[None], (at, 0, 0))

        def slot(s, up):
            if up:
                return jnp.where(z + s < n_z, z + s, z)
            return jnp.where(z >= s, z - s, z)

        below, above = line(up_own)
        rows = up_own.shape[0]
        up = jnp.zeros((n_fs,) + up_own.shape, BF16)
        up_y = send(up_own, over_y)
        for s in range(1, n_z):
            from_lo = send(below[s], y_where(lambda zz: zz >= s))
            from_hi = send(above[s], y_where(lambda zz: zz <= n_z - 1 - s))
            up = put(up, below[s], slot(s, False) * 2 + y)
            up = put(up, above[s], slot(s, True) * 2 + y)
            up = put(up, from_lo, slot(s, False) * 2 + 1 - y)
            up = put(up, from_hi, slot(s, True) * 2 + 1 - y)
        up = put(up, up_own, z * 2 + y)
        up = put(up, up_y, z * 2 + 1 - y)
        up_ready = up.reshape(n_fs * rows, -1)
        down_own = after(down_own, below[2], above[2])

        tok_x = send(tokens, over_x)
        tok_c = send(tokens, over_c)
        tok_xc = send(tok_x, over_c)

        def place(own, dx, dc, dxc):
            lo, hi = jnp.where(x == 0, own, dx), jnp.where(x == 0, dx, own)
            lo_c, hi_c = jnp.where(x == 0, dc, dxc), jnp.where(x == 0, dxc, dc)
            return [jnp.where(c == 0, lo, lo_c), jnp.where(c == 0, lo_c, lo),
                    jnp.where(c == 0, hi, hi_c), jnp.where(c == 0, hi_c, hi)]

        normed = normalize(jnp.concatenate(place(tokens, tok_x, tok_c, tok_xc), axis=1))
        before = jnp.dot(normed, up_ready, preferred_element_type=F32)
        hidden = jnp.square(jax.nn.relu(before)).astype(BF16)
        half = hidden.shape[1] // 2
        hid_own = jnp.where(y == 0, hidden[:, :half], hidden[:, half:])
        hid_oth = jnp.where(y == 0, hidden[:, half:], hidden[:, :half])

        width = down_own.shape[1] // 2
        halves = [line(down_own[:, h * width:(h + 1) * width]) for h in range(2)]
        mixed, down, far_sent = [], [], None
        for h, (below, above) in enumerate(halves):
            own = below[0]
            buf = jnp.zeros((n_z,) + own.shape, BF16)
            for s in range(1, n_z):
                buf = put(buf, below[s], slot(s, False))
                buf = put(buf, above[s], slot(s, True))
            buf = put(buf, own, z)
            if h:
                buf, hid_own, hid_oth = lax.optimization_barrier((buf, hid_own, hid_oth))

            def rows_of(at):
                return lax.dynamic_slice(buf, (at, 0, 0), (1,) + own.shape)[0]

            x_me = send(rows_of(2 * (1 - x) + c), over_x)
            x_co = send(rows_of(2 * (1 - x) + 1 - c), over_x)
            near = {(0, 0): rows_of(2 * x + c), (0, 1): send(rows_of(2 * x + 1 - c), over_c),
                    (1, 0): x_me, (1, 1): send(x_co, over_c)}
            away = {k: send(v, over_y) for k, v in near.items()}
            if h:
                keys = list(away)
                away = dict(zip(keys, lax.optimization_barrier(tuple(away[k] for k in keys) + (far_sent,))))

            def part(k):
                return (jnp.dot(hid_own, near[k], preferred_element_type=F32)
                        + jnp.dot(hid_oth, away[k], preferred_element_type=F32))

            far = part((1, 0)) + send(part((1, 1)).astype(BF16), over_c).astype(F32)
            far_sent = far.astype(BF16)
            far = send(far_sent, over_x)
            mine = part((0, 0)) + send(part((0, 1)).astype(BF16), over_c).astype(F32)
            mixed.append((mine + far.astype(F32)).astype(BF16))

            order = [(0, 0), (1, 0), (0, 1), (1, 1)]
            mine_rows = place(*[near[k] for k in order])
            oth_rows = place(*[away[k] for k in order])
            down.append([jnp.concatenate([jnp.where(y == 0, m, o), jnp.where(y == 0, o, m)], axis=0)
                         for m, o in zip(mine_rows, oth_rows)])
        down_ready = jnp.concatenate([d[t_at] for t_at in range(n_tp) for d in down], axis=1)
        return jnp.concatenate(mixed, axis=1), up_ready, down_ready

    return shards


def solution(mesh):
    n_fs, n_tp = mesh.shape["fs"], mesh.shape["tp"]
    small = n_tp == 4 and n_fs == 2 * n_tp
    return jax.shard_map(
        routed(n_fs, n_tp) if small else plain,
        mesh=mesh,
        in_specs=(P("fs", "tp"), P("fs"), P("fs", "tp"), P("fs", "tp")),
        out_specs=(P("fs", "tp"), P(None, "tp"), P("tp", None)),
        check_vma=False,
    )
```

```python
import jax
import jax.numpy as jnp
from jax import lax
from jax.sharding import PartitionSpec as P


AXES = ("fs", "tp")
BF16, F32 = jnp.bfloat16, jnp.float32


def plain(tokens, norm_gain, up_master, down_master):
    up_local = (norm_gain[:, None] * up_master).astype(BF16)
    up_ready = lax.all_gather(up_local, "fs", axis=0, tiled=True)
    gathered = lax.all_gather(down_master.astype(BF16), "fs", axis=0, tiled=True)
    down_ready = lax.all_to_all(gathered, "tp", split_axis=0, concat_axis=1, tiled=True)
    normed = normalize(lax.all_gather(tokens, "tp", axis=1, tiled=True))
    before = jnp.dot(normed, up_ready, preferred_element_type=F32)
    hidden = jnp.square(jax.nn.relu(before)).astype(BF16)
    part = jnp.dot(hidden, down_ready, preferred_element_type=F32).astype(BF16)
    mixed = lax.psum_scatter(part, "tp", scatter_dimension=1, tiled=True)
    return mixed, up_ready, down_ready


def normalize(features):
    values = features.astype(F32)
    mean_square = jnp.mean(values * values, axis=-1, keepdims=True)
    return (values * lax.rsqrt(mean_square + 1e-06)).astype(BF16)


def routed(n_fs, n_tp):
    n_z = n_fs // 2

    def pairs(move):
        out = []
        for s in range(n_fs * n_tp):
            f, t = divmod(s, n_tp)
            to = move(f // 2, f % 2, t // 2, t % 2)
            if to is not None:
                z, y, x, c = to
                out.append((s, (z * 2 + y) * n_tp + x * 2 + c))
        return out

    over_x = pairs(lambda z, y, x, c: (z, y, 1 - x, c))
    over_y = pairs(lambda z, y, x, c: (z, 1 - y, x, c))
    over_c = pairs(lambda z, y, x, c: (z, y, x, 1 - c))

    def send(value, route):
        return lax.ppermute(value, AXES, route)

    def y_where(keep):
        return pairs(lambda z, y, x, c: (z, 1 - y, x, c) if keep(z) else None)

    def rising(step):
        return pairs(lambda z, y, x, c: (z + 1, y, x, c) if step - 1 <= z < n_z - 1 else None)

    def falling(step):
        return pairs(lambda z, y, x, c: (z - 1, y, x, c) if 1 <= z <= n_z - step else None)

    def shards(tokens, norm_gain, up_master, down_master):
        f, t = lax.axis_index("fs"), lax.axis_index("tp")
        z, y, x, c = f // 2, f % 2, t // 2, t % 2

        up_own = (norm_gain[:, None] * up_master).astype(BF16)
        down_own = down_master.astype(BF16)

        def step_of(line, step):
            line[0].append(send(line[0][-1], rising(step)))
            line[1].append(send(line[1][-1], falling(step)))

        def gate(line, *others):
            ends = lax.optimization_barrier((line[0][-1], line[1][-1]) + others)
            line[0][-1], line[1][-1] = ends[:2]

        def put(buf, value, at):
            return lax.dynamic_update_slice(buf, value[None], (at, 0, 0))

        def slot(s, up):
            if up:
                return jnp.where(z + s < n_z, z + s, z)
            return jnp.where(z >= s, z - s, z)

        last = n_z - 1
        width = down_own.shape[1] // 2
        lines = [([v], [v]) for v in (up_own, down_own[:, :width], down_own[:, width:])]

        def ends(k):
            return lines[k][0][-1], lines[k][1][-1]

        step_of(lines[0], 1)
        for step in range(1, last):
            gate(lines[1], *ends(0))
            step_of(lines[0], step + 1)
            step_of(lines[1], step)
        gate(lines[1], *ends(0))
        gate(lines[2], *ends(1))
        step_of(lines[1], last)
        step_of(lines[2], 1)
        for step in range(2, n_z):
            gate(lines[2], *ends(1))
            step_of(lines[2], step)
        below, above = lines[0]
        rows = up_own.shape[0]
        up = jnp.zeros((n_fs,) + up_own.shape, BF16)
        up_y = send(up_own, over_y)
        for s in range(1, n_z):
            from_lo = send(below[s], y_where(lambda zz: zz >= s))
            from_hi = send(above[s], y_where(lambda zz: zz <= n_z - 1 - s))
            up = put(up, below[s], slot(s, False) * 2 + y)
            up = put(up, above[s], slot(s, True) * 2 + y)
            up = put(up, from_lo, slot(s, False) * 2 + 1 - y)
            up = put(up, from_hi, slot(s, True) * 2 + 1 - y)
        up = put(up, up_own, z * 2 + y)
        up = put(up, up_y, z * 2 + 1 - y)
        up_ready = up.reshape(n_fs * rows, -1)

        tok_x = send(tokens, over_x)
        tok_c = send(tokens, over_c)
        tok_xc = send(tok_x, over_c)

        def place(own, dx, dc, dxc):
            lo, hi = jnp.where(x == 0, own, dx), jnp.where(x == 0, dx, own)
            lo_c, hi_c = jnp.where(x == 0, dc, dxc), jnp.where(x == 0, dxc, dc)
            return [jnp.where(c == 0, lo, lo_c), jnp.where(c == 0, lo_c, lo),
                    jnp.where(c == 0, hi, hi_c), jnp.where(c == 0, hi_c, hi)]

        normed = normalize(jnp.concatenate(place(tokens, tok_x, tok_c, tok_xc), axis=1))
        before = jnp.dot(normed, up_ready, preferred_element_type=F32)
        hidden = jnp.square(jax.nn.relu(before)).astype(BF16)
        half = hidden.shape[1] // 2
        hid_own = jnp.where(y == 0, hidden[:, :half], hidden[:, half:])
        hid_oth = jnp.where(y == 0, hidden[:, half:], hidden[:, :half])

        mixed, down, far_sent = [], [], None
        for h, (below, above) in enumerate(lines[1:]):
            own = below[0]
            buf = jnp.zeros((n_z,) + own.shape, BF16)
            for s in range(1, n_z):
                buf = put(buf, below[s], slot(s, False))
                buf = put(buf, above[s], slot(s, True))
            buf = put(buf, own, z)
            if h:
                buf, hid_own, hid_oth = lax.optimization_barrier((buf, hid_own, hid_oth))

            def rows_of(at):
                return lax.dynamic_slice(buf, (at, 0, 0), (1,) + own.shape)[0]

            x_me = send(rows_of(2 * (1 - x) + c), over_x)
            x_co = send(rows_of(2 * (1 - x) + 1 - c), over_x)
            keep_me, keep_co = rows_of(2 * x + c), rows_of(2 * x + 1 - c)
            if h:
                x_me, x_co, keep_me, keep_co = lax.optimization_barrier((x_me, x_co, keep_me, keep_co))
            near = {(1, 0): x_me, (1, 1): send(x_co, over_c),
                    (0, 0): keep_me, (0, 1): send(keep_co, over_c)}
            away = {k: send(v, over_y) for k, v in near.items()}
            if h:
                keys = list(away)
                away = dict(zip(keys, lax.optimization_barrier(tuple(away[k] for k in keys) + (far_sent,))))

            def part(k):
                return (jnp.dot(hid_own, near[k], preferred_element_type=F32)
                        + jnp.dot(hid_oth, away[k], preferred_element_type=F32))

            far = part((1, 0)) + send(part((1, 1)).astype(BF16), over_c).astype(F32)
            far_sent = far.astype(BF16)
            far = send(far_sent, over_x)
            mine = part((0, 0)) + send(part((0, 1)).astype(BF16), over_c).astype(F32)
            mixed.append((mine + far.astype(F32)).astype(BF16))

            order = [(0, 0), (1, 0), (0, 1), (1, 1)]
            mine_rows = place(*[near[k] for k in order])
            oth_rows = place(*[away[k] for k in order])
            down.append([jnp.concatenate([jnp.where(y == 0, m, o), jnp.where(y == 0, o, m)], axis=0)
                         for m, o in zip(mine_rows, oth_rows)])
        down_ready = jnp.concatenate([d[t_at] for t_at in range(n_tp) for d in down], axis=1)
        return jnp.concatenate(mixed, axis=1), up_ready, down_ready

    return shards


def solution(mesh):
    n_fs, n_tp = mesh.shape["fs"], mesh.shape["tp"]
    small = n_tp == 4 and n_fs == 2 * n_tp
    return jax.shard_map(
        routed(n_fs, n_tp) if small else plain,
        mesh=mesh,
        in_specs=(P("fs", "tp"), P("fs"), P("fs", "tp"), P("fs", "tp")),
        out_specs=(P("fs", "tp"), P(None, "tp"), P("tp", None)),
        check_vma=False,
    )
```

```python
import jax
import jax.numpy as jnp
from jax import lax
from jax.sharding import PartitionSpec as P


AXES = ("fs", "tp")
BF16, F32 = jnp.bfloat16, jnp.float32


def plain(tokens, norm_gain, up_master, down_master):
    up_local = (norm_gain[:, None] * up_master).astype(BF16)
    up_ready = lax.all_gather(up_local, "fs", axis=0, tiled=True)
    gathered = lax.all_gather(down_master.astype(BF16), "fs", axis=0, tiled=True)
    down_ready = lax.all_to_all(gathered, "tp", split_axis=0, concat_axis=1, tiled=True)
    normed = normalize(lax.all_gather(tokens, "tp", axis=1, tiled=True))
    before = jnp.dot(normed, up_ready, preferred_element_type=F32)
    hidden = jnp.square(jax.nn.relu(before)).astype(BF16)
    part = jnp.dot(hidden, down_ready, preferred_element_type=F32).astype(BF16)
    mixed = lax.psum_scatter(part, "tp", scatter_dimension=1, tiled=True)
    return mixed, up_ready, down_ready


def normalize(features):
    values = features.astype(F32)
    mean_square = jnp.mean(values * values, axis=-1, keepdims=True)
    return (values * lax.rsqrt(mean_square + 1e-06)).astype(BF16)


def routed(n_fs, n_tp):
    n_z = n_fs // 2

    def pairs(move):
        out = []
        for s in range(n_fs * n_tp):
            f, t = divmod(s, n_tp)
            to = move(f // 2, f % 2, t // 2, t % 2)
            if to is not None:
                z, y, x, c = to
                out.append((s, (z * 2 + y) * n_tp + x * 2 + c))
        return out

    over_x = pairs(lambda z, y, x, c: (z, y, 1 - x, c))
    over_y = pairs(lambda z, y, x, c: (z, 1 - y, x, c))
    over_c = pairs(lambda z, y, x, c: (z, y, x, 1 - c))

    def send(value, route):
        return lax.ppermute(value, AXES, route)

    def y_where(keep):
        return pairs(lambda z, y, x, c: (z, 1 - y, x, c) if keep(z) else None)

    def rising(step):
        return pairs(lambda z, y, x, c: (z + 1, y, x, c) if step - 1 <= z < n_z - 1 else None)

    def falling(step):
        return pairs(lambda z, y, x, c: (z - 1, y, x, c) if 1 <= z <= n_z - step else None)

    def shards(tokens, norm_gain, up_master, down_master):
        f, t = lax.axis_index("fs"), lax.axis_index("tp")
        z, y, x, c = f // 2, f % 2, t // 2, t % 2

        up_own = (norm_gain[:, None] * up_master).astype(BF16)
        down_own = down_master.astype(BF16)

        def step_of(line, step):
            line[0].append(send(line[0][-1], rising(step)))
            line[1].append(send(line[1][-1], falling(step)))

        def gate(line, *others):
            ends = lax.optimization_barrier((line[0][-1], line[1][-1]) + others)
            line[0][-1], line[1][-1] = ends[:2]

        def put(buf, value, at):
            return lax.dynamic_update_slice(buf, value[None], (at, 0, 0))

        def slot(s, up):
            if up:
                return jnp.where(z + s < n_z, z + s, z)
            return jnp.where(z >= s, z - s, z)

        last = n_z - 1
        width = down_own.shape[1] // 2
        lines = [([v], [v]) for v in (up_own, down_own[:, :width], down_own[:, width:])]

        def ends(k):
            return lines[k][0][-1], lines[k][1][-1]

        step_of(lines[0], 1)
        for step in range(1, last):
            gate(lines[1], *ends(0))
            step_of(lines[0], step + 1)
            step_of(lines[1], step)
        gate(lines[1], *ends(0))
        gate(lines[2], *ends(1))
        step_of(lines[1], last)
        step_of(lines[2], 1)
        for step in range(2, n_z):
            gate(lines[2], *ends(1))
            step_of(lines[2], step)
        below, above = lines[0]
        rows = up_own.shape[0]
        up = jnp.zeros((n_fs,) + up_own.shape, BF16)
        up_y = send(up_own, over_y)
        for s in range(1, n_z):
            from_lo = send(below[s], y_where(lambda zz: zz >= s))
            from_hi = send(above[s], y_where(lambda zz: zz <= n_z - 1 - s))
            up = put(up, below[s], slot(s, False) * 2 + y)
            up = put(up, above[s], slot(s, True) * 2 + y)
            up = put(up, from_lo, slot(s, False) * 2 + 1 - y)
            up = put(up, from_hi, slot(s, True) * 2 + 1 - y)
        up = put(up, up_own, z * 2 + y)
        up = put(up, up_y, z * 2 + 1 - y)
        up_ready = up.reshape(n_fs * rows, -1)

        tok_x = send(tokens, over_x)
        tok_c = send(tokens, over_c)
        tok_xc = send(tok_x, over_c)

        def place(own, dx, dc, dxc):
            lo, hi = jnp.where(x == 0, own, dx), jnp.where(x == 0, dx, own)
            lo_c, hi_c = jnp.where(x == 0, dc, dxc), jnp.where(x == 0, dxc, dc)
            return [jnp.where(c == 0, lo, lo_c), jnp.where(c == 0, lo_c, lo),
                    jnp.where(c == 0, hi, hi_c), jnp.where(c == 0, hi_c, hi)]

        normed = normalize(jnp.concatenate(place(tokens, tok_x, tok_c, tok_xc), axis=1))
        before = jnp.dot(normed, up_ready, preferred_element_type=F32)
        hidden = jnp.square(jax.nn.relu(before)).astype(BF16)
        half = hidden.shape[1] // 2
        hid_own = jnp.where(y == 0, hidden[:, :half], hidden[:, half:])
        hid_oth = jnp.where(y == 0, hidden[:, half:], hidden[:, :half])

        mixed, down, far_sent = [], [], None
        for h, (below, above) in enumerate(lines[1:]):
            own = below[0]
            buf = jnp.zeros((n_z,) + own.shape, BF16)
            for s in range(1, n_z):
                buf = put(buf, below[s], slot(s, False))
                buf = put(buf, above[s], slot(s, True))
            buf = put(buf, own, z)

            def rows_of(at):
                return lax.dynamic_slice(buf, (at, 0, 0), (1,) + own.shape)[0]

            x_me = send(rows_of(2 * (1 - x) + c), over_x)
            x_co = send(rows_of(2 * (1 - x) + 1 - c), over_x)
            keep_me, keep_co = rows_of(2 * x + c), rows_of(2 * x + 1 - c)
            if h:
                x_me, x_co, keep_me, keep_co, hid_own, hid_oth = lax.optimization_barrier(
                    (x_me, x_co, keep_me, keep_co, hid_own, hid_oth))
            near = {(1, 0): x_me, (1, 1): send(x_co, over_c),
                    (0, 0): keep_me, (0, 1): send(keep_co, over_c)}
            away = {k: send(v, over_y) for k, v in near.items()}
            if h:
                keys = list(away)
                away = dict(zip(keys, lax.optimization_barrier(tuple(away[k] for k in keys) + (far_sent,))))

            def part(k):
                return (jnp.dot(hid_own, near[k], preferred_element_type=F32)
                        + jnp.dot(hid_oth, away[k], preferred_element_type=F32))

            far = part((1, 0)) + send(part((1, 1)).astype(BF16), over_c).astype(F32)
            far_sent = far.astype(BF16)
            far = send(far_sent, over_x)
            mine = part((0, 0)) + send(part((0, 1)).astype(BF16), over_c).astype(F32)
            mixed.append((mine + far.astype(F32)).astype(BF16))

            order = [(0, 0), (1, 0), (0, 1), (1, 1)]
            mine_rows = place(*[near[k] for k in order])
            oth_rows = place(*[away[k] for k in order])
            down.append([jnp.concatenate([jnp.where(y == 0, m, o), jnp.where(y == 0, o, m)], axis=0)
                         for m, o in zip(mine_rows, oth_rows)])
        down_ready = jnp.concatenate([d[t_at] for t_at in range(n_tp) for d in down], axis=1)
        return jnp.concatenate(mixed, axis=1), up_ready, down_ready

    return shards


def solution(mesh):
    n_fs, n_tp = mesh.shape["fs"], mesh.shape["tp"]
    small = n_tp == 4 and n_fs == 2 * n_tp
    return jax.shard_map(
        routed(n_fs, n_tp) if small else plain,
        mesh=mesh,
        in_specs=(P("fs", "tp"), P("fs"), P("fs", "tp"), P("fs", "tp")),
        out_specs=(P("fs", "tp"), P(None, "tp"), P("tp", None)),
        check_vma=False,
    )
```
